256 devices in a mesh: ep: 64 (over z, x, core), tp: 4 (over y).
Axes of the slice: x: 4, y: 4, z: 8, core: 2. Of those that a mesh axis runs over, the one named last changes fastest.
Arguments:
- gate_branch: bfloat16 [32768, 2048], P(('ep', 'tp')), may hold values from -8 to 8
- rec_branch: bfloat16 [32768, 2048], P(('ep', 'tp')), may hold values from -6 to 6
- conv_weight: float32 [4, 2048], replicated, may hold values from -3 to 3
- gate_a: bfloat16 [8, 256, 256], replicated, may hold values from -0.375 to 0.375
- gate_x: bfloat16 [8, 256, 256], replicated, may hold values from -0.375 to 0.375
- decay_param: float32 [2048], replicated, as said below
- decay_shift: float32 [32768], P(('ep', 'tp')), may hold values from -0.6 to 0
- tokens: bfloat16 [32768, 2048], P(('ep', 'tp')), may hold values from -6 to 6
- routes: int32 [32768, 2], P(('ep', 'tp')), may hold values from 0 to 63, all different within a row; in each aligned block of 128 rows (0 to 127, 128 to 255, ...) at most 5 rows name the same one
- route_weight: float32 [32768, 2], P(('ep', 'tp')), may hold values from 0.1 to 0.9
- norm_gain: float32 [2048], replicated, may hold values from 0.1 to 1.9
- w_gate: bfloat16 [64, 2048, 3584], P('ep', None, 'tp'), may hold values from -0.125 to 0.125
- w_up: bfloat16 [64, 2048, 3584], P('ep', None, 'tp'), may hold values from -0.125 to 0.125
- w_down: bfloat16 [64, 3584, 2048], P('ep', 'tp'), may hold values from -0.09375 to 0.09375
Outputs:
- mixed_out: bfloat16 [32768, 2048], P(('ep', 'tp'))
- expert_out: bfloat16 [32768, 2048], P(('ep', 'tp'))
The draws below stay inside these ranges and needn't reach their ends.
Inputs may be any that keep to these rules, and one draw needn't show every extreme that they name: `routes`: in each aligned block of 128 rows (the rows of one device) no expert is named more than 5 times, and some block names some expert exactly 5 times; the experts of one row differ. 8 softplus(-decay_param) lies between 0.2 / 32768 and 0.07.
All inputs are finite; a program needn't handle non-finite values.
Results may differ from the reference program's by a relative error of at most 0.012.
Values may be sent and summed in bfloat16 or wider, within the bound.
A program may use at most 128 MiB of HBM per device.

```python
import math
import jax
import jax.numpy as jnp
import numpy as np
from jax import lax

D = 2048
BLOCK = 256
BLOCKS = 8
TAPS = 4
FF = 3584
TOPK = 2
A_ROWS = 128
B_ROWS = 128
EXPERTS = 64
CAP = 5
TOK_A = 32768
TOK_B = 32768
N_TP = 4


def draw_decay_param(key, part):
    keys = jax.random.split(key, 3)
    fast = jax.random.uniform(keys[0], (D,), jnp.float32) < 0.5
    fast_rate = jnp.exp(jax.random.uniform(keys[1], (D,), jnp.float32, jnp.log(0.02), jnp.log(0.07)))
    slow_rate = jnp.exp(jax.random.uniform(keys[2], (D,), jnp.float32, jnp.log(0.2), jnp.log(1.0))) / TOK_A
    decay_rate = jnp.where(fast, fast_rate, slow_rate)
    return -jnp.log(jnp.expm1(decay_rate / 8.0))


def draw_decay_shift(key, part):
    keys = jax.random.split(key, 3)
    block_count = TOK_A // A_ROWS
    level = jnp.exp(jax.random.uniform(keys[0], (block_count,), jnp.float32, jnp.log(0.05), jnp.log(0.6))) / TOK_A
    shift_rows = -jnp.repeat(level, A_ROWS)
    spots = jax.random.randint(keys[1], (2,), 0, TOK_A)
    depth = jax.random.uniform(keys[2], (2,), jnp.float32, -0.5, -0.22)
    return shift_rows.at[spots].add(depth)


def levels(stream_key, dims, pieces, low, high):
    def one(position, shards_of):
        steps = jax.random.uniform(jax.random.fold_in(jax.random.fold_in(stream_key, 6), position), (shards_of,), jnp.float32, low / len(pieces), high / len(pieces))
        return jnp.repeat(jnp.exp(steps), dims[position] // shards_of).reshape((-1,) + (1,) * (len(dims) - position - 1))

    loudness = one(*pieces[0])
    for cut in pieces[1:]:
        loudness = loudness * one(*cut)
    return loudness


def shared_out(key, own, number, rows, amount, top, most, lean):
    order = jax.random.permutation(key, amount)
    packed, common = load_shares(amount, rows * top, most, lean, True), load_shares(amount, rows * top, most, lean, False)
    places = jnp.arange(amount)

    def named(sizes, turn):
        used = int((sizes > 0).sum())
        fixed = max(1, used // 4)
        moved = fixed + (places - fixed + turn * (used - fixed)) % max(1, amount - fixed)
        return jnp.zeros((amount,), jnp.int32).at[order[jnp.where(places < fixed, places, moved)]].set(jnp.asarray(sizes, jnp.int32))

    sizes = jnp.where(number % 4 == 0, named(packed, number // 4), named(common, number - number // 4 - 1))
    mixed = jax.random.permutation(jax.random.fold_in(own, 3), amount)
    donor, taker = mixed[0:amount // 2 * 2:2], mixed[1:amount // 2 * 2:2]
    margin = jnp.minimum(sizes[donor] - 1, most - sizes[taker]) // 2
    margin = jnp.where((donor == order[0]) | (taker == order[0]) | (sizes[taker] == 0), 0, jnp.maximum(margin, 0))
    moved = jax.random.randint(jax.random.fold_in(own, 4), (amount // 2,), 0, 1 << 20) % (margin + 1)
    sizes = sizes.at[donor].add(-moved).at[taker].add(moved)
    members = jnp.searchsorted(jnp.cumsum(sizes), jnp.arange(rows * top), side="right").astype(jnp.int32)
    listing = members.reshape(top, rows).T
    listing = listing[jax.random.permutation(jax.random.fold_in(own, 1), rows)]
    turn = jax.random.randint(jax.random.fold_in(own, 2), (rows, 1), 0, top)
    return jnp.take_along_axis(listing, (jnp.arange(top)[None, :] + turn) % top, axis=1)


def load_shares(amount, total, bound, skew, full):
    portions = [(1 << 20) // math.isqrt(grade ** skew) + 1 for grade in range(1, amount + 1)]
    largest = bound if full else min(bound, max(-(-total // amount), total * portions[0] // sum(portions)))
    least = 1 if total - largest >= amount - 1 else 0
    counts, surplus = [largest] + [least] * (amount - 1), total - largest - least * (amount - 1)
    while surplus > 0:
        movable = [i for i in range(1, amount) if counts[i] < largest] or [i for i in range(1, amount) if counts[i] < bound]
        mass, budget = sum([portions[i] for i in movable]), surplus
        for i in movable:
            addition = min(bound - counts[i], max(1, budget * portions[i] // mass), surplus)
            counts[i] = counts[i] + addition
            surplus = surplus - addition
    return np.array(counts)


def scatter_about(own_key, dims, width, most, cuts=(), kind=jnp.bfloat16):
    values = jax.random.normal(own_key, dims, jnp.float32) * width
    if len(cuts) > 0:
        values = levels(own_key, dims, cuts, -0.22, 0.18) * values
    return jnp.clip(values, min=-most, max=most).astype(kind)


def setup_inputs(seed: int = 0) -> dict:
    seeds = jax.random.split(jax.random.key(seed), 15)
    gate_branch = scatter_about(seeds[0], (TOK_A, D), 1.5, 8.0, ((0, 256),))
    rec_branch = scatter_about(seeds[1], (TOK_A, D), 1.0, 6.0, ((0, 256),))
    conv_weight = scatter_about(seeds[2], (TAPS, D), TAPS ** -0.5, 3.0, (), jnp.float32)
    gate_a = scatter_about(seeds[3], (BLOCKS, BLOCK, BLOCK), BLOCK ** -0.5, 0.375)
    gate_x = scatter_about(seeds[4], (BLOCKS, BLOCK, BLOCK), BLOCK ** -0.5, 0.375)
    decay_param = draw_decay_param(jax.random.fold_in(seeds[14], 71), 0)
    decay_shift = draw_decay_shift(jax.random.fold_in(seeds[14], 71), 0)
    tokens = scatter_about(seeds[7], (TOK_B, D), 1.0, 6.0, ((0, 256),))
    routes_keys = jax.random.split(jax.random.fold_in(seeds[8], 1), TOK_B // B_ROWS)
    routes_turns = jax.random.permutation(jax.random.fold_in(seeds[8], 3), TOK_B // B_ROWS)
    routes = jax.vmap(lambda own, number: shared_out(jax.random.fold_in(seeds[8], 2), own, number, B_ROWS, EXPERTS, TOPK, CAP, 2))(routes_keys, routes_turns).reshape((TOK_B, TOPK))
    route_weight = jnp.clip(0.1 + 0.79999997 * jax.random.uniform(seeds[9], (TOK_B, TOPK), jnp.float32) ** levels(seeds[9], (TOK_B, TOPK), ((0, 256),), -0.2, 0.2), 0.1, 0.9)
    norm_gain = jnp.clip(1.0 + 0.18 * jax.random.normal(seeds[10], (D,), jnp.float32), 0.1, 1.9)
    w_gate = scatter_about(seeds[11], (EXPERTS, D, FF), D ** -0.5, 0.125, ((0, 64), (2, 4)))
    w_up = scatter_about(seeds[12], (EXPERTS, D, FF), D ** -0.5, 0.125, ((0, 64), (2, 4)))
    w_down = scatter_about(seeds[13], (EXPERTS, FF, D), FF ** -0.5, 0.09375, ((0, 64), (1, 4)))
    return {"gate_branch": gate_branch, "rec_branch": rec_branch, "conv_weight": conv_weight, "gate_a": gate_a, "gate_x": gate_x, "decay_param": decay_param, "decay_shift": decay_shift, "tokens": tokens, "routes": routes, "route_weight": route_weight, "norm_gain": norm_gain, "w_gate": w_gate, "w_up": w_up, "w_down": w_down}


EPSILON = 1e-05

def pair_combine(earlier, later):
    return (earlier[0] * later[0], later[0] * earlier[1] + later[1])

def short_conv(previous, current, conv_weight):
    tap_count = conv_weight.shape[0]
    row_count = current.shape[0]
    padded = jnp.concatenate([previous, current], 0)
    summed = jnp.zeros(current.shape, jnp.float32)
    for tap_index in range(tap_count):
        summed = summed + conv_weight[tap_index] * padded[tap_index:tap_index + row_count].astype(jnp.float32)
    return summed.astype(jnp.bfloat16)

def mixer_gates(conv_rows, gate_a, gate_x, decay_rate, shift_rows):
    row_count, width_all = conv_rows.shape
    block_count, block_width = (gate_a.shape[0], gate_a.shape[1])
    split_rows = conv_rows.reshape(row_count, block_count, block_width).astype(jnp.float32)
    pre_a = jnp.einsum('rnc,ncd->rnd', split_rows, gate_a.astype(jnp.float32))
    pre_x = jnp.einsum('rnc,ncd->rnd', split_rows, gate_x.astype(jnp.float32))
    recur_gate = jax.nn.sigmoid(pre_a.reshape(row_count, width_all))
    input_gate = jax.nn.sigmoid(pre_x.reshape(row_count, width_all))
    log_a = -decay_rate[None, :] * recur_gate + shift_rows[:, None]
    drive = jnp.sqrt(-jnp.expm1(2.0 * log_a)) * input_gate * conv_rows.astype(jnp.float32)
    return (log_a, drive)

def mixer_reference(gate_branch, rec_branch, conv_weight, gate_a, gate_x, decay_param, decay_shift):
    total_rows, width_all = rec_branch.shape
    tap_count = conv_weight.shape[0]
    leading = jnp.zeros((tap_count - 1, width_all), jnp.bfloat16)
    conv_rows = short_conv(leading, rec_branch, conv_weight)
    decay_rate = 8.0 * jax.nn.softplus(-decay_param)
    span_rows = 512 if total_rows % 512 == 0 else total_rows
    span_count = total_rows // span_rows

    def advance(carried, span_index):
        start_row = span_index * span_rows
        conv_span = lax.dynamic_slice_in_dim(conv_rows, start_row, span_rows, 0)
        gate_span = lax.dynamic_slice_in_dim(gate_branch, start_row, span_rows, 0)
        shift_span = lax.dynamic_slice_in_dim(decay_shift, start_row, span_rows, 0)
        log_a, drive = mixer_gates(conv_span, gate_a, gate_x, decay_rate, shift_span)
        factor, local_state = lax.associative_scan(pair_combine, (jnp.exp(log_a), drive), axis=0)
        states = local_state + factor * carried[None, :]
        mixed = (states * jax.nn.gelu(gate_span.astype(jnp.float32), approximate=True)).astype(jnp.bfloat16)
        return (states[-1], mixed)
    start_state = jnp.zeros((width_all,), jnp.float32)
    _, mixed_spans = lax.scan(advance, start_state, jnp.arange(span_count, dtype=jnp.int32))
    return mixed_spans.reshape(total_rows, width_all)

def layer_scale(rows_in, norm_gain):
    values = rows_in.astype(jnp.float32)
    center = lax.optimization_barrier(jnp.mean(values, -1, keepdims=True))
    spread = lax.optimization_barrier(jnp.mean(jnp.square(values - center), -1, keepdims=True))
    return ((values - center) * lax.rsqrt(spread + EPSILON) * norm_gain).astype(jnp.bfloat16)

def slot_numbers(routes, block_rows, expert_count):
    row_count, top_count = routes.shape
    onehot = (routes[:, :, None] == jnp.arange(expert_count, dtype=jnp.int32)).astype(jnp.int32)
    ranked = jnp.cumsum(onehot.reshape(row_count // block_rows, block_rows * top_count, expert_count), axis=1) - 1
    return lax.optimization_barrier(jnp.sum(ranked.reshape(row_count, top_count, expert_count) * onehot, -1)).astype(jnp.int32)

def expert_result(rows_in, gate_full, up_full, down_full, shard_count):
    hidden = (jax.nn.silu(jnp.dot(rows_in, gate_full, preferred_element_type=jnp.float32)) * jnp.dot(rows_in, up_full, preferred_element_type=jnp.float32)).astype(jnp.bfloat16)
    unit_count = hidden.shape[1] // shard_count
    summed = jnp.zeros((rows_in.shape[0], down_full.shape[1]), jnp.float32)
    for shard_index in range(shard_count):
        lower = shard_index * unit_count
        piece = jnp.dot(hidden[:, lower:lower + unit_count], down_full[lower:lower + unit_count], preferred_element_type=jnp.float32).astype(jnp.bfloat16)
        piece = lax.optimization_barrier(piece)
        summed = summed + piece.astype(jnp.float32)
    return summed.astype(jnp.bfloat16)

def experts_reference(tokens, routes, route_weight, norm_gain, w_gate, w_up, w_down):
    row_count, width_all = tokens.shape
    expert_count = w_gate.shape[0]
    capacity = CAP
    block_count = row_count // B_ROWS
    normed = layer_scale(tokens, norm_gain)
    slots = slot_numbers(routes, B_ROWS, expert_count)
    row_ids = jnp.broadcast_to(jnp.arange(row_count, dtype=jnp.int32)[:, None], routes.shape)
    flat = (row_ids // B_ROWS * expert_count + routes) * capacity + slots
    table_size = block_count * expert_count * capacity
    table = jnp.full((table_size,), row_count, jnp.int32).at[flat.reshape(-1)].set(row_ids.reshape(-1))
    weight_table = jnp.zeros((table_size,), jnp.float32).at[flat.reshape(-1)].set(route_weight.reshape(-1))
    table = table.reshape(block_count, expert_count, capacity)
    weight_table = weight_table.reshape(block_count, expert_count, capacity)

    def add_expert(summed, expert_index):
        picks = jnp.take(table, expert_index, axis=1).reshape(-1)
        weights = jnp.take(weight_table, expert_index, axis=1).reshape(-1)
        rows_in = jnp.take(normed, picks, axis=0, mode='fill', fill_value=0)
        result = expert_result(rows_in, w_gate[expert_index], w_up[expert_index], w_down[expert_index], N_TP)
        summed = summed.at[picks].add(weights[:, None] * result.astype(jnp.float32), mode='drop')
        return (summed, None)
    start_sum = jnp.zeros((row_count, width_all), jnp.float32)
    summed, _ = lax.scan(add_expert, start_sum, jnp.arange(expert_count, dtype=jnp.int32))
    return summed.astype(jnp.bfloat16)

def reference(gate_branch, rec_branch, conv_weight, gate_a, gate_x, decay_param, decay_shift, tokens, routes, route_weight, norm_gain, w_gate, w_up, w_down):
    mixed_out = mixer_reference(gate_branch, rec_branch, conv_weight, gate_a, gate_x, decay_param, decay_shift)
    expert_out = experts_reference(tokens, routes, route_weight, norm_gain, w_gate, w_up, w_down)
    return (mixed_out, expert_out)
```

```python
import functools

import jax
import jax.numpy as jnp
from jax import lax
from jax.experimental import pallas as pl
from jax.experimental.pallas import tpu as pltpu
from jax.sharding import Mesh
from jax.sharding import PartitionSpec as P

AXES = ("ep_0", "ep_1", "ep_2", "tp")
EP = ("ep_0", "ep_1", "ep_2")
MESH = pl.DeviceIdType.MESH
EPSILON = 1e-05
CAP = 5
F32 = jnp.float32
BF16 = jnp.bfloat16


def iota(shape, dim):
    return lax.broadcasted_iota(jnp.int32, shape, dim)


def mm(a, b):
    return jnp.dot(a, b, preferred_element_type=F32)


def minus_expm1(x):
    series = 1.0 + x * (1.0 / 7.0)
    for k in (6.0, 5.0, 4.0, 3.0, 2.0):
        series = 1.0 + x * (1.0 / k) * series
    return -jnp.where(x > -0.25, x * series, jnp.exp(x) - 1.0)


def kernel(
    zn, xn, cn, tpn,
    tok, gain, routes, rw, rate, shift, convw,
    rec_h, gate_h, ga_h, gx_h, wg_h, wu_h, wd_h,
    mixed_o, expert_o,
    wgu, wd, ga, gx, rec, gate, halo, hist, dec, sta,
    out, zr, tt, xx, part, ra, rb, rc, cs, rr, rt, rz, ret, hid, whl, acc,
    tot1, tot2, tot3,
    ld, halo_s, halo_r,
    z_s, z_r, x_s, x_r, bx_s, bx_r, bz_s, bz_r,
    y_s, y_r, c1_s, c1_r, c2_s, c2_r, c3_s, c3_r,
):
    xcn = xn * cn
    en = zn * xcn
    z, x, c, tp = (lax.axis_index(name) for name in AXES)
    xc = x * cn + c
    rows, width = tok.shape
    ff = wd.shape[0]
    half = en // 2

    def at_z(k):
        return (lax.rem(z + k, zn), x, c, tp)

    def at_xc(dx, dc):
        return (z, lax.rem(x + dx, xn), lax.rem(c + dc, cn), tp)

    def at_tp(k):
        return (z, x, c, lax.rem(tp + k, tpn))

    def at_xc_abs(k):
        return (z, k // cn, lax.rem(k, cn), tp)

    plus, minus = at_tp(1), at_tp(tpn - 1)
    total = en * tpn
    me = ((z * xn + x) * cn + c) * tpn + tp

    def at_flat(i):
        e = i // tpn
        return (e // xcn, lax.rem(e // cn, xn), lax.rem(e, cn), lax.rem(i, tpn))

    follower, leader = at_flat(lax.rem(me + 1, total)), at_flat(lax.rem(me + total - 1, total))

    def rcopy(src, dst, ss, rs, dev):
        return pltpu.make_async_remote_copy(
            src_ref=src, dst_ref=dst, send_sem=ss, recv_sem=rs, device_id=dev, device_id_type=MESH
        )

    def loop(lo, hi, body):
        def step(i, carry):
            body(i)
            return carry

        lax.fori_loop(lo, hi, step, 0)

    loads = [
        pltpu.make_async_copy(rec_h, rec, ld.at[0]),
        pltpu.make_async_copy(ga_h, ga, ld.at[1]),
        pltpu.make_async_copy(gx_h, gx, ld.at[2]),
        pltpu.make_async_copy(gate_h, gate, ld.at[3]),
        pltpu.make_async_copy(wd_h.at[0], wd, ld.at[4]),
    ]
    for copy in loads:
        copy.start()

    def gu_copy(j, which):
        source = wg_h if which == 0 else wu_h
        return pltpu.make_async_copy(
            source.at[0, :, pl.ds(j * 128, 128)],
            wgu.at[:, pl.ds(j * 256 + which * 128, 128)],
            ld.at[5 + 2 * j + which],
        )

    for j in range(ff // 128):
        gu_copy(j, 0).start()
        gu_copy(j, 1).start()

    barrier = pltpu.get_barrier_semaphore()

    def greet(dev):
        pl.semaphore_signal(barrier, inc=1, device_id=dev, device_id_type=MESH)

    loop(1, zn, lambda k: greet(at_z(k)))
    loop(1, xcn, lambda k: greet(at_xc(k // cn, lax.rem(k, cn))))
    loop(1, tpn, lambda k: greet(at_tp(k)))
    greet(follower)
    greet(leader)

    values = tok[...].astype(F32)
    center = jnp.mean(values, -1, keepdims=True)
    values = values - center
    spread = jnp.mean(jnp.square(values), -1, keepdims=True)
    normed = (values * lax.rsqrt(spread + EPSILON) * gain[...]).astype(BF16)

    eye = iota((rows, rows), 0) == iota((rows, rows), 1)
    before = (iota((rows, rows), 1) < iota((rows, rows), 0)).astype(F32).astype(BF16)
    experts = iota((rows, en), 1)
    picked = [routes[:, k : k + 1] == experts for k in range(2)]
    ones = [p.astype(F32) for p in picked]
    ranks = [mm(before, o.astype(BF16)) for o in ones]
    ranks[1] = ranks[1] + jnp.sum(ones[0], axis=0, keepdims=True)
    place_col, place_row = [], []
    lc, lx = cn.bit_length() - 1, xn.bit_length() - 1
    for k in range(2):
        slot = jnp.sum(ones[k] * ranks[k], axis=1, keepdims=True)
        e = routes[:, k : k + 1]
        dz = ((e >> (lc + lx)) - z) & (zn - 1)
        dx = ((e >> lc) - x) & (xn - 1)
        dc = (e - c) & (cn - 1)
        col = slot * float(en) + (dz * xcn + dx * cn + dc).astype(F32)
        place_col.append(col)
        place_row.append(jnp.sum(jnp.where(eye, col, 0.0), axis=0, keepdims=True))
    pl.semaphore_wait(barrier, zn + xcn + tpn - 3 + 2)

    loads[0].wait()
    halo_copy = rcopy(rec.at[pl.ds(rows - 8, 8)], halo, halo_s.at[0], halo_r.at[0], follower)
    halo_copy.start()

    def z_copy(s, k):
        span = pl.ds(pl.multiple_of(k * xcn, xcn), xcn)
        return rcopy(out.at[s, span], zr.at[s, span], z_s.at[s, k], z_r.at[s, k], at_z(k))

    spots = iota((en, rows), 0).astype(F32)
    for s in range(CAP):
        base = spots + float(s * en)
        take = jnp.where((place_row[0] == base) | (place_row[1] == base), 1.0, 0.0).astype(BF16)
        out[s] = mm(take, normed).astype(BF16)
        loop(1, zn, lambda k, s=s: z_copy(s, k).start())
    lane = iota((rows, 2 * en), 1)
    spot = (lane & (en - 1)).astype(F32)
    for s in range(CAP):
        base = spot + float(s * en)
        weight = jnp.where(place_col[0] == base, rw[:, 0:1], 0.0)
        weight = weight + jnp.where(place_col[1] == base, rw[:, 1:2], 0.0)
        high = weight.astype(BF16).astype(F32)
        whl[s] = jnp.where(lane < en, high, weight - high).astype(BF16)

    shift_col = jnp.sum(jnp.where(eye, shift[...], 0.0), axis=1, keepdims=True)
    loads[1].wait()
    loads[2].wait()
    halo_copy.wait()
    hist[8:, :] = rec[...].astype(F32)
    hist[0:8, :] = jnp.where(me == 0, 0.0, halo[...].astype(F32))
    steps = rows // 8

    def mixer_block(b):
        cols = pl.ds(pl.multiple_of(b * 256, 256), 256)
        conv = jnp.zeros((rows, 256), F32)
        for j in range(4):
            conv = conv + convw[j : j + 1, cols] * hist[5 + j : 5 + j + rows, cols]
        conv = conv.astype(BF16)
        recur = jax.nn.sigmoid(mm(conv, ga[b]))
        enter = jax.nn.sigmoid(mm(conv, gx[b]))
        log_a = shift_col - rate[:, cols] * recur
        decay = jnp.exp(log_a)
        drive = jnp.sqrt(minus_expm1(2.0 * log_a)) * enter * conv.astype(F32)
        for h in range(2):
            n = 2 * b + h
            dec[n] = decay[:, h * 128 : h * 128 + 128]
            sta[n] = drive[:, h * 128 : h * 128 + 128]
            factor, state = dec[n, pl.ds(0, 8, stride=steps)], sta[n, pl.ds(0, 8, stride=steps)]
            for i in range(1, steps):
                at = pl.ds(i, 8, stride=steps)
                a = dec[n, at]
                state = a * state + sta[n, at]
                factor = factor * a
                dec[n, at] = factor
                sta[n, at] = state
            f, t = factor[0:1], state[0:1]
            for g in range(1, 8):
                t = factor[g : g + 1] * t + state[g : g + 1]
                f = factor[g : g + 1] * f
            lanes = pl.ds(pl.multiple_of(n * 128, 128), 128)
            tot1[tp, 0:1, lanes] = f
            tot1[tp, 1:2, lanes] = t

    loop(0, width // 256, mixer_block)

    def t1_copy(k):
        return rcopy(tot1.at[tp], tot1.at[tp], c1_s.at[k], c1_r.at[tp], at_tp(k))

    def t1_wait(k):
        far = lax.rem(tp + k, tpn)
        rcopy(tot1.at[far], tot1.at[far], c1_s.at[k], c1_r.at[far], at_tp(k)).wait_recv()

    def t2_copy(k):
        return rcopy(
            tot2.at[xc], tot2.at[xc], c2_s.at[k], c2_r.at[xc], at_xc_abs(lax.rem(xc + k, xcn))
        )

    def t2_wait(k):
        far = lax.rem(xc + k, xcn)
        rcopy(tot2.at[far], tot2.at[far], c2_s.at[k], c2_r.at[far], at_xc_abs(far)).wait_recv()

    def t3_copy(k):
        return rcopy(tot3.at[z], tot3.at[z], c3_s.at[k], c3_r.at[z], at_z(k))

    def t3_wait(k):
        far = lax.rem(z + k, zn)
        rcopy(tot3.at[far], tot3.at[far], c3_s.at[k], c3_r.at[far], at_z(k)).wait_recv()

    loop(1, tpn, lambda k: t1_copy(k).start())

    def fold(ref, count, here):
        f, t = jnp.ones((1, width), F32), jnp.zeros((1, width), F32)
        fi, ti = f, t
        for k in range(count):
            a, b = ref[k, 0:1, :], ref[k, 1:2, :]
            t = a * t + b
            f = f * a
            inside = k < here
            fi = jnp.where(inside, f, fi)
            ti = jnp.where(inside, t, ti)
        return (f, t), (fi, ti)

    swap_in = iota((en, en), 1) == (iota((en, en), 0) & (zn - 1)) * xcn + (
        iota((en, en), 0) >> (zn.bit_length() - 1)
    )
    swap_in = swap_in.astype(F32).astype(BF16)
    swap_out = iota((en, en), 1) == (iota((en, en), 0) & (xcn - 1)) * zn + (
        iota((en, en), 0) >> (xcn.bit_length() - 1)
    )
    swap_out = swap_out.astype(F32).astype(BF16)

    def x_copy(s, k):
        span = pl.ds(pl.multiple_of(k * zn, zn), zn)
        return rcopy(
            tt.at[s, span], xx.at[s, span], x_s.at[s, k], x_r.at[s, k],
            at_xc(k // cn, lax.rem(k, cn)),
        )

    def bx_copy(s, k):
        span = pl.ds(pl.multiple_of(k * zn, zn), zn)
        return rcopy(
            rr.at[s, span], rt.at[s, span], bx_s.at[s, k], bx_r.at[s, k],
            at_xc(xn - k // cn, cn - lax.rem(k, cn)),
        )

    def bz_copy(s, k):
        span = pl.ds(pl.multiple_of(k * xcn, xcn), xcn)
        return rcopy(rz.at[s, span], ret.at[s, span], bz_s.at[s, k], bz_r.at[s, k], at_z(zn - k))

    def y_copy(s, number):
        def block(b, side):
            return pl.ds(b * en + side * half, half)

        src, dst, dev = {
            0: (xx.at[s, pl.ds(0, en)], xx.at[s, pl.ds(3 * en, en)], plus),
            1: (xx.at[s, pl.ds(0, en)], xx.at[s, pl.ds(en, en)], minus),
            2: (xx.at[s, block(3, 0)], xx.at[s, block(2, 0)], plus),
            3: (xx.at[s, block(1, 1)], xx.at[s, block(2, 1)], minus),
            4: (part.at[s, block(2, 0)], ra.at[s, 0], plus),
            5: (part.at[s, block(2, 1)], ra.at[s, 1], minus),
            6: (part.at[s, block(1, 1)], rb.at[s, 0], plus),
            7: (part.at[s, block(3, 0)], rb.at[s, 1], minus),
            8: (cs.at[s, 0], rc.at[s, 0], plus),
            9: (cs.at[s, 1], rc.at[s, 1], minus),
        }[number]
        return rcopy(src, dst, y_s.at[s, number], y_r.at[s, number], dev)

    def stage0(s):
        loop(1, zn, lambda k: z_copy(s, k).wait_recv())
        zr[s, 0:xcn] = out[s, 0:xcn]
        tt[s] = mm(swap_in, zr[s]).astype(BF16)
        loop(1, xcn, lambda k: x_copy(s, k).start())
        xx[s, 0:zn] = tt[s, 0:zn]

    def stage1(s):
        loop(1, xcn, lambda k: x_copy(s, k).wait_recv())
        y_copy(s, 0).start()
        y_copy(s, 1).start()

    def stage2(s):
        y_copy(s, 0).wait_recv()
        y_copy(s, 2).start()
        y_copy(s, 1).wait_recv()
        y_copy(s, 3).start()

    def stage3(s):
        y_copy(s, 2).wait_recv()
        y_copy(s, 3).wait_recv()

        def up(j):
            pair = mm(xx[s], wgu[:, pl.ds(pl.multiple_of(j * 256, 256), 256)])
            gated, raised = pair[:, :128], pair[:, 128:]
            cols = pl.ds(pl.multiple_of(j * 128, 128), 128)
            hid[:, cols] = (gated * jax.nn.sigmoid(gated) * raised).astype(BF16)

        loop(0, ff // 128, up)

        def down(j):
            cols = pl.ds(pl.multiple_of(j * 256, 256), 256)
            part[s, :, cols] = mm(hid[...], wd[:, cols]).astype(BF16)

        loop(0, width // 256, down)
        for number in (4, 5, 6, 7):
            y_copy(s, number).start()

    def stage4(s):
        for side, b in ((0, 1), (1, 3)):
            y_copy(s, 4 + side).wait_recv()
            mine = part[s, b * en + side * half : b * en + side * half + half]
            cs[s, side] = (ra[s, side].astype(F32) + mine.astype(F32)).astype(BF16)
            y_copy(s, 8 + side).start()

    def stage5(s):
        for number in (6, 7, 8, 9):
            y_copy(s, number).wait_recv()
        for side in range(2):
            mine = part[s, side * half : side * half + half].astype(F32)
            mine = mine + rc[s, side].astype(F32) + rb[s, 1 - side].astype(F32)
            rr[s, side * half : side * half + half] = mine.astype(BF16)
        loop(1, xcn, lambda k: bx_copy(s, k).start())
        rt[s, 0:zn] = rr[s, 0:zn]

    def stage6(s):
        loop(1, xcn, lambda k: bx_copy(s, k).wait_recv())
        rz[s] = mm(swap_out, rt[s]).astype(BF16)
        loop(1, zn, lambda k: bz_copy(s, k).start())
        ret[s, 0:xcn] = rz[s, 0:xcn]

    def stage7(s):
        loop(1, zn, lambda k: bz_copy(s, k).wait_recv())
        back = ret[s]
        acc[...] += mm(whl[s], jnp.concatenate([back, back], 0))

    acc[...] = jnp.zeros_like(acc)
    stages = ((0, stage0), (1, stage1), (2, stage2), (4, stage4), (5, stage5), (6, stage6),
              (7, stage7), (3, stage3))

    def carry_1():
        loop(1, tpn, t1_wait)
        (f, t), _ = fold(tot1, tpn, tp)
        tot2[xc, 0:1, :] = f
        tot2[xc, 1:2, :] = t
        loop(1, xcn, lambda k: t2_copy(k).start())

    def carry_2():
        loop(1, xcn, t2_wait)
        (f, t), _ = fold(tot2, xcn, xc)
        tot3[z, 0:1, :] = f
        tot3[z, 1:2, :] = t
        loop(1, zn, lambda k: t3_copy(k).start())

    def carry_3():
        loop(1, zn, t3_wait)
        _, (_, t3) = fold(tot3, zn, z)
        _, (f2, t2) = fold(tot2, xcn, xc)
        _, (f1, t1) = fold(tot1, tpn, tp)
        hist[0:1, :] = f1 * (f2 * t3 + t2) + t1
        loads[3].wait()

        def finish(n):
            cols = pl.ds(pl.multiple_of(n * 128, 128), 128)
            last = pl.ds(steps - 1, 8, stride=steps)
            factor, state = dec[n, last], sta[n, last]
            starts = [hist[0:1, cols]]
            for g in range(7):
                starts.append(factor[g : g + 1] * starts[-1] + state[g : g + 1])
            start = jnp.concatenate(starts, 0)
            for i in range(steps):
                at = pl.ds(i, 8, stride=steps)
                sta[n, at] = sta[n, at] + dec[n, at] * start
            mixed_o[:, cols] = (
                sta[n] * jax.nn.gelu(gate[:, cols].astype(F32), approximate=True)
            ).astype(BF16)

        loop(0, width // 128, finish)

    def tick(t):
        for number, stage in stages:
            if number == 3:
                @pl.when(t == 3)
                def _():
                    for j in range(ff // 128):
                        gu_copy(j, 0).wait()
                        gu_copy(j, 1).wait()
                    loads[4].wait()

            pl.when((t >= number) & (t < number + CAP))(functools.partial(stage, t - number))
        pl.when(t == 1)(carry_1)
        pl.when(t == 2)(carry_2)
        pl.when(t == 7)(carry_3)

    loop(0, CAP + 7, tick)
    expert_o[...] = acc[...].astype(BF16)

    loop(1, tpn, lambda k: t1_copy(k).wait_send())
    loop(1, xcn, lambda k: t2_copy(k).wait_send())
    loop(1, zn, lambda k: t3_copy(k).wait_send())

    def drain(s):
        loop(1, zn, lambda k: z_copy(s, k).wait_send())
        loop(1, xcn, lambda k: x_copy(s, k).wait_send())
        loop(1, xcn, lambda k: bx_copy(s, k).wait_send())
        loop(1, zn, lambda k: bz_copy(s, k).wait_send())
        for number in range(10):
            y_copy(s, number).wait_send()

    loop(0, CAP, drain)


def shards(
    gate_branch, rec_branch, conv_weight, gate_a, gate_x, decay_param, decay_shift,
    tokens, routes, route_weight, norm_gain, w_gate, w_up, w_down,
):
    zn, xn, cn, tpn = (lax.axis_size(name) for name in AXES)
    en = zn * xn * cn
    rows, width = tokens.shape
    ff = w_gate.shape[2]
    rate = (8.0 * jax.nn.softplus(-decay_param)).reshape(1, width)
    vmem = pl.BlockSpec(memory_space=pltpu.VMEM)
    hbm = pl.BlockSpec(memory_space=pl.ANY)
    dma = pltpu.SemaphoreType.DMA
    scratch = [
        pltpu.VMEM((width, 2 * ff), BF16), pltpu.VMEM((ff, width), BF16),
        pltpu.VMEM(gate_a.shape, BF16), pltpu.VMEM(gate_x.shape, BF16),
        pltpu.VMEM((rows, width), BF16), pltpu.VMEM((rows, width), BF16),
        pltpu.VMEM((8, width), BF16), pltpu.VMEM((rows + 8, width), F32),
        pltpu.VMEM((width // 128, rows, 128), F32), pltpu.VMEM((width // 128, rows, 128), F32),
        pltpu.VMEM((CAP, en, width), BF16), pltpu.VMEM((CAP, en, width), BF16),
        pltpu.VMEM((CAP, en, width), BF16), pltpu.VMEM((CAP, 4 * en, width), BF16),
        pltpu.VMEM((CAP, 4 * en, width), BF16),
        pltpu.VMEM((CAP, 2, en // 2, width), BF16), pltpu.VMEM((CAP, 2, en // 2, width), BF16),
        pltpu.VMEM((CAP, 2, en // 2, width), BF16), pltpu.VMEM((CAP, 2, en // 2, width), BF16),
        pltpu.VMEM((CAP, en, width), BF16), pltpu.VMEM((CAP, en, width), BF16),
        pltpu.VMEM((CAP, en, width), BF16), pltpu.VMEM((CAP, en, width), BF16),
        pltpu.VMEM((4 * en, ff), BF16), pltpu.VMEM((CAP, rows, 2 * en), BF16),
        pltpu.VMEM((rows, width), F32),
        pltpu.VMEM((tpn, 2, width), F32), pltpu.VMEM((xn * cn, 2, width), F32),
        pltpu.VMEM((zn, 2, width), F32),
        dma((5 + 2 * (ff // 128),)), dma((1,)), dma((1,)),
        dma((CAP, zn)), dma((CAP, zn)), dma((CAP, xn * cn)), dma((CAP, xn * cn)),
        dma((CAP, xn * cn)), dma((CAP, xn * cn)), dma((CAP, zn)), dma((CAP, zn)),
        dma((CAP, 10)), dma((CAP, 10)),
        dma((tpn,)), dma((tpn,)), dma((xn * cn,)), dma((xn * cn,)), dma((zn,)), dma((zn,)),
    ]
    shape = jax.ShapeDtypeStruct((rows, width), BF16)
    return pl.pallas_call(
        functools.partial(kernel, zn, xn, cn, tpn),
        out_shape=(shape, shape),
        in_specs=[vmem] * 7 + [hbm] * 7,
        out_specs=(vmem, vmem),
        scratch_shapes=scratch,
        compiler_params=pltpu.CompilerParams(
            collective_id=0, has_side_effects=True, vmem_limit_bytes=64 * 1024 * 1024 - 65536
        ),
    )(
        tokens, norm_gain.reshape(1, width), routes, route_weight, rate,
        decay_shift.reshape(1, rows), conv_weight,
        rec_branch, gate_branch, gate_a, gate_x, w_gate, w_up, w_down,
    )


def solution(mesh):
    shape = (8, 4, 2, mesh.shape["tp"])
    split = Mesh(mesh.devices.reshape(shape), AXES)
    return jax.shard_map(
        shards,
        mesh=split,
        in_specs=(
            P(AXES, None), P(AXES, None), P(), P(), P(), P(), P(AXES),
            P(AXES, None), P(AXES, None), P(AXES, None), P(),
            P(EP, None, "tp"), P(EP, None, "tp"), P(EP, "tp", None),
        ),
        out_specs=(P(AXES, None), P(AXES, None)),
        check_vma=False,
    )
```
